32 devices in a mesh: grp: 2 (over y), sp: 4 (over z), tp: 4 (over x, core).
Axes of the slice: x: 2, y: 2, z: 4, core: 2. Of those that a mesh axis runs over, the one named last changes fastest.
Arguments:
- query_rows: bfloat16 [4096, 1024], P(('grp', 'sp'), 'tp'), parts along dimension 0, may hold values from -128 to 128
- key_rows: bfloat16 [4096, 256], P(('grp', 'sp'), 'tp'), parts along dimension 0, may hold values from -4 to 4
- value_rows: bfloat16 [4096, 256], P(('grp', 'sp'), 'tp'), parts along dimension 0, may hold values from -6 to 6
- sink_logits: float32 [16], P('tp'), may hold values from 3 to 7
- residual: bfloat16 [4096, 2048], P(('grp', 'sp', 'tp')), parts along dimension 0, may hold values from -6 to 6
- out_weight: bfloat16 [1024, 2048], P('tp'), may hold values from -0.1875 to 0.1875
- norm_gain: float32 [2048], replicated, may hold values from 0.1 to 1.9
- gate_weight: bfloat16 [16, 2048, 512], P(('sp', 'tp')), may hold values from -0.125 to 0.125
- up_weight: bfloat16 [16, 2048, 512], P(('sp', 'tp')), may hold values from -0.125 to 0.125
- down_weight: bfloat16 [16, 512, 2048], P(('sp', 'tp')), may hold values from -0.25 to 0.25
- routes: int32 [4096, 2], P(('grp', 'sp', 'tp')), parts along dimension 0, may hold values from 0 to 15, as said below
- route_weight: float32 [4096, 2], P(('grp', 'sp', 'tp')), parts along dimension 0, may hold values from 0.1 to 1
Outputs:
- layer_out: bfloat16 [4096, 2048], P(('grp', 'sp', 'tp')), parts along dimension 0
The draws below stay inside these ranges and needn't reach their ends.
There are 2 independent parts, one for each index of `grp`. The reference program is written for one: setup_inputs(seed, part) draws one part's arguments, and reference() takes and returns one part's arrays. A program takes and returns all parts, laid end to end along the dimension named above; an argument that names none is the same for every part. Nothing has to cross between parts.
Inputs may be any that keep to these rules, and one draw needn't show every extreme that they name: `routes`: A token's two experts differ and lie in the same group of 4 consecutive experts. Among the 128 tokens of one device (aligned blocks of 128 rows) no expert is named more than 32 times; in every block each expert of one group, the same group for all blocks, is named exactly 32 times.
All inputs are finite; a program needn't handle non-finite values.
Results may differ from the reference program's by a relative error of at most 0.013.
Values may be sent and summed in bfloat16 or wider, within the bound.
No kernel may reach another device: no remote copies, remote signals or barrier semaphores. Data moves between devices by JAX's collectives and lax.ppermute only.
A program may use at most 64 MiB of HBM per device.

```python
import math
import jax
import jax.numpy as jnp
from jax import lax

D = 2048
HEADS = 16
KV = 4
HDIM = 64
WINDOW = 128
FFE = 512
GROUPS = 4
TOKENS = 2048
ROWS = 128
EXPERTS = 16
EPG = 4
CAP = 32


def shared_rows(key):
    key_part = jnp.clip(jax.random.normal(jax.random.fold_in(key, 1), (TOKENS, KV * HDIM), jnp.float32), -4.0, 4.0)
    query_part = jnp.clip(jax.random.normal(jax.random.fold_in(key, 2), (TOKENS, HEADS * HDIM), jnp.float32), -4.0, 4.0)
    return (query_part, key_part)


def draw_query_rows(key, part):
    query_part, key_part = shared_rows(jax.random.fold_in(key, 17))
    return query_part.astype(jnp.bfloat16)


def draw_key_rows(key, part):
    query_part, key_part = shared_rows(jax.random.fold_in(key, 17))
    return key_part.astype(jnp.bfloat16)


def draw_routes(key, part):
    block_count = TOKENS // ROWS
    half_rows = ROWS // 2
    full_group = jax.random.randint(jax.random.fold_in(key, 5), (), 0, GROUPS)

    def one_block(block_key):
        cuts = jnp.sort(jax.random.randint(jax.random.fold_in(block_key, 1), (GROUPS - 2,), 0, half_rows + 1))
        bounds = jnp.concatenate([jnp.zeros((1,), jnp.int32), cuts.astype(jnp.int32), jnp.full((1,), half_rows, jnp.int32)])
        other_sizes = bounds[1:] - bounds[:-1]
        others = (full_group + 1 + jnp.arange(GROUPS - 1, dtype=jnp.int32)) % GROUPS
        sizes = jnp.zeros((GROUPS,), jnp.int32).at[others].set(other_sizes).at[full_group].set(half_rows)
        ends = jnp.cumsum(sizes)
        starts = ends - sizes
        order = jax.random.permutation(jax.random.fold_in(block_key, 2), ROWS)
        places = jnp.arange(ROWS, dtype=jnp.int32)
        group_of = jnp.sum((places[:, None] >= ends[None, :]).astype(jnp.int32), axis=1)
        within = places - starts[group_of]
        group_keys = jax.vmap(lambda g: jax.random.fold_in(block_key, 10 + g))(jnp.arange(GROUPS, dtype=jnp.int32))
        perms = jax.vmap(lambda k: jax.random.permutation(k, EPG))(group_keys).astype(jnp.int32)
        offset = 1 + within // EPG % (EPG - 1)
        first_local = perms[group_of, within % EPG]
        second_local = perms[group_of, (within + offset) % EPG]
        pair = jnp.stack([group_of * EPG + first_local, group_of * EPG + second_local], axis=1).astype(jnp.int32)
        return jnp.zeros((ROWS, 2), jnp.int32).at[order].set(pair)
    block_keys = jax.vmap(lambda b: jax.random.fold_in(key, 100 + b))(jnp.arange(block_count, dtype=jnp.int32))
    return jax.vmap(one_block)(block_keys).reshape(TOKENS, 2)


def block_levels(own_key, extent, split, smallest, top_value):
    def one(axis_at, blocks):
        heights = jax.random.uniform(jax.random.fold_in(jax.random.fold_in(own_key, 6), axis_at), (blocks,), jnp.float32, smallest / len(split), top_value / len(split))
        return jnp.repeat(jnp.exp(heights), extent[axis_at] // blocks).reshape((-1,) + (1,) * (len(extent) - axis_at - 1))

    level = one(*split[0])
    for cut in split[1:]:
        level = level * one(*cut)
    return level


def normal_values(own_key, extent, scale, limit, shards=(), kind=jnp.bfloat16):
    entries = scale * jax.random.normal(own_key, extent, jnp.float32)
    if shards:
        entries = entries * block_levels(own_key, extent, shards, -0.22, 0.18)
    return jnp.clip(entries, -limit, limit).astype(kind)


def setup_inputs(seed: int = 0, part: int = 0) -> dict:
    keys = jax.random.split(jax.random.key(seed), 13)
    part_splits = jax.random.split(jax.random.fold_in(keys[12], part), 13)
    query_rows = draw_query_rows(jax.random.fold_in(jax.random.fold_in(keys[12], part), 71), part)
    key_rows = draw_key_rows(jax.random.fold_in(jax.random.fold_in(keys[12], part), 71), part)
    value_rows = normal_values(part_splits[2], (TOKENS, KV * HDIM), 1.0, 6.0, ((0, 4), (1, 4)))
    sink_logits = jnp.clip(3.0 + 4.0 * jax.random.uniform(keys[3], (HEADS,), jnp.float32) ** block_levels(keys[3], (HEADS,), ((0, 4),), -0.2, 0.2), 3.0, 7.0)
    residual = normal_values(part_splits[4], (TOKENS, D), 1.0, 6.0, ((0, 16),))
    out_weight = normal_values(keys[5], (HEADS * HDIM, D), (HEADS * HDIM) ** -0.5, 0.1875, ((0, 4),))
    norm_gain = jnp.clip(1.0 + 0.18 * jax.random.normal(keys[6], (D,), jnp.float32), 0.1, 1.9)
    gate_weight = normal_values(keys[7], (EXPERTS, D, FFE), D ** -0.5, 0.125, ((0, 16),))
    up_weight = normal_values(keys[8], (EXPERTS, D, FFE), D ** -0.5, 0.125, ((0, 16),))
    down_weight = normal_values(keys[9], (EXPERTS, FFE, D), FFE ** -0.5, 0.25, ((0, 16),))
    routes = draw_routes(jax.random.fold_in(jax.random.fold_in(keys[12], part), 71), part)
    route_weight = jnp.clip(jnp.exp(math.log(1.0) - 2.3025851 * jax.random.uniform(part_splits[11], (TOKENS, 2), jnp.float32) ** block_levels(part_splits[11], (TOKENS, 2), ((0, 16),), -0.2, 0.2)), 0.1, 1.0)
    return {"query_rows": query_rows, "key_rows": key_rows, "value_rows": value_rows, "sink_logits": sink_logits, "residual": residual, "out_weight": out_weight, "norm_gain": norm_gain, "gate_weight": gate_weight, "up_weight": up_weight, "down_weight": down_weight, "routes": routes, "route_weight": route_weight}


rope_base = 10000.0
norm_eps = 1e-06

def rotate(rows, positions, heads):
    half_dim = HDIM // 2
    values = rows.astype(jnp.float32).reshape(rows.shape[0], heads, HDIM)
    inverse = rope_base ** (-jnp.arange(half_dim, dtype=jnp.float32) / half_dim)
    angles = positions.astype(jnp.float32)[:, None] * inverse[None, :]
    cosines = jnp.cos(angles)[:, None, :]
    sines = jnp.sin(angles)[:, None, :]
    lower = values[..., :half_dim]
    upper = values[..., half_dim:]
    turned = jnp.concatenate([lower * cosines - upper * sines, upper * cosines + lower * sines], axis=-1)
    return turned.reshape(rows.shape[0], heads * HDIM).astype(jnp.bfloat16)

def reference(query_rows, key_rows, value_rows, sink_logits, residual, out_weight, norm_gain, gate_weight, up_weight, down_weight, routes, route_weight):
    positions = jnp.arange(TOKENS, dtype=jnp.int32)
    rot_q = rotate(query_rows, positions, HEADS)
    rot_k = rotate(key_rows, positions, KV)
    repeat = HEADS // KV
    blocks = TOKENS // WINDOW
    q_blocks = rot_q.reshape(blocks, WINDOW, KV, repeat, HDIM)
    k_blocks = rot_k.reshape(blocks, WINDOW, KV, HDIM)
    v_blocks = value_rows.reshape(blocks, WINDOW, KV, HDIM)
    k_wide = jnp.concatenate([jnp.concatenate([jnp.zeros_like(k_blocks[:1]), k_blocks[:-1]], axis=0), k_blocks], axis=1)
    v_wide = jnp.concatenate([jnp.concatenate([jnp.zeros_like(v_blocks[:1]), v_blocks[:-1]], axis=0), v_blocks], axis=1)
    query_pos = jnp.arange(WINDOW) + WINDOW
    key_pos = jnp.arange(2 * WINDOW)
    distance = query_pos[:, None] - key_pos[None, :]
    in_band = (distance >= 0) & (distance < WINDOW)
    earliest = (jnp.arange(blocks)[:, None, None] > 0) | (key_pos[None, None, :] >= WINDOW)
    allowed = in_band[None] & earliest
    sinks_grouped = sink_logits.astype(jnp.float32).reshape(KV, repeat)

    def one_group(group):
        q_group = q_blocks[:, :, group].astype(jnp.float32)
        k_group = k_wide[:, :, group].astype(jnp.float32)
        v_group = v_wide[:, :, group].astype(jnp.float32)
        scores = jnp.einsum('nqrd,nkd->rnqk', q_group, k_group) * HDIM ** (-0.5)
        scores = jnp.where(allowed[None], scores, -jnp.inf)
        sink_here = sinks_grouped[group][:, None, None, None]
        largest = jnp.maximum(scores.max(axis=-1, keepdims=True), sink_here)
        exp_scores = jnp.exp(scores - largest)
        denominator = exp_scores.sum(axis=-1, keepdims=True) + jnp.exp(sink_here - largest)
        probs = (exp_scores / denominator).astype(jnp.bfloat16)
        mixed = jnp.einsum('rnqk,nkd->nqrd', probs.astype(jnp.float32), v_group)
        return mixed.astype(jnp.bfloat16)
    attended = lax.map(one_group, jnp.arange(KV, dtype=jnp.int32))
    attended = attended.transpose(1, 2, 0, 3, 4).reshape(TOKENS, HEADS * HDIM)
    projected = jnp.dot(attended, out_weight, preferred_element_type=jnp.float32)
    stream = (residual.astype(jnp.float32) + projected).astype(jnp.bfloat16)
    stream_f = stream.astype(jnp.float32)
    normed = (stream_f * lax.rsqrt(lax.optimization_barrier(jnp.mean(stream_f * stream_f, axis=-1, keepdims=True)) + norm_eps) * norm_gain[None, :]).astype(jnp.bfloat16)
    flat_expert = routes.reshape(-1).astype(jnp.int32)
    token_of = (jnp.arange(2 * TOKENS, dtype=jnp.int32) // 2).astype(jnp.int32)
    one_hot = (flat_expert[:, None] == jnp.arange(EXPERTS, dtype=jnp.int32)[None, :]).astype(jnp.int32)
    slot_rank = lax.optimization_barrier(jnp.sum((jnp.cumsum(one_hot, axis=0) - one_hot) * one_hot, axis=1)).astype(jnp.int32)
    slots = EXPERTS * CAP
    index_table = jnp.full((EXPERTS, slots), TOKENS, jnp.int32).at[flat_expert, slot_rank].set(token_of)
    weight_table = jnp.zeros((EXPERTS, slots), jnp.float32).at[flat_expert, slot_rank].set(route_weight.reshape(-1).astype(jnp.float32))
    padded = jnp.concatenate([normed, jnp.zeros((1, D), jnp.bfloat16)], axis=0)

    def serve(total, expert):
        picked = index_table[expert]
        routed = padded[picked]
        gate_out = jnp.dot(routed, gate_weight[expert], preferred_element_type=jnp.float32)
        up_out = jnp.dot(routed, up_weight[expert], preferred_element_type=jnp.float32)
        hidden = (jax.nn.silu(gate_out) * up_out).astype(jnp.bfloat16)
        expert_out = jnp.dot(hidden, down_weight[expert], preferred_element_type=jnp.float32).astype(jnp.bfloat16)
        total = total.at[picked].add(weight_table[expert][:, None] * expert_out.astype(jnp.float32))
        return (total, None)
    summed, _ = lax.scan(serve, jnp.zeros((TOKENS + 1, D), jnp.float32), jnp.arange(EXPERTS, dtype=jnp.int32))
    return (stream_f + summed[:TOKENS]).astype(jnp.bfloat16)
```

```python
import jax
import jax.numpy as jnp
from jax import lax
from jax.sharding import PartitionSpec as P

HDIM = 64
WINDOW = 128


rope_base = 10000.0
norm_eps = 1e-06


def shifted(block, axis, distance):
    devices = range(lax.axis_size(axis))
    route = [(i - distance, i) for i in devices if i - distance in devices]
    return lax.ppermute(block, axis, route)


def swapped(block, axis, offset):
    return lax.ppermute(block, axis, [(i, i ^ offset) for i in range(lax.axis_size(axis))])


def gathered_by_doubling(block, axis):
    blocks = {0: block}
    offset = lax.axis_size(axis) // 2
    while offset:
        blocks.update({m ^ offset: swapped(b, axis, offset) for m, b in blocks.items()})
        offset //= 2
    return blocks


def slots_of(routes, expert_count, capacity):
    count = routes.shape[0]
    experts = jnp.arange(expert_count, dtype=jnp.int32)
    named = (routes[:, :, None] == experts[None, None, :]).astype(jnp.bfloat16)
    either = named[:, 0] + named[:, 1]
    row = jnp.arange(count, dtype=jnp.int32)
    earlier = (row[:, None] > row[None, :]).astype(jnp.bfloat16)
    before = jnp.dot(earlier, either, preferred_element_type=jnp.float32)
    rank = jnp.sum(before[:, None, :] * named.astype(jnp.float32), axis=-1).astype(jnp.int32)
    return routes * capacity + rank


def rotate(rows, positions, heads):
    half_dim = HDIM // 2
    values = rows.astype(jnp.float32).reshape(rows.shape[0], heads, HDIM)
    inverse = rope_base ** (-jnp.arange(half_dim, dtype=jnp.float32) / half_dim)
    angles = positions.astype(jnp.float32)[:, None] * inverse[None, :]
    cosines = jnp.cos(angles)[:, None, :]
    sines = jnp.sin(angles)[:, None, :]
    lower = values[..., :half_dim]
    upper = values[..., half_dim:]
    turned = jnp.concatenate(
        [lower * cosines - upper * sines, upper * cosines + lower * sines], axis=-1
    )
    return turned.reshape(rows.shape[0], heads * HDIM).astype(jnp.bfloat16)


def per_device(
    query_rows,
    key_rows,
    value_rows,
    sink_logits,
    residual,
    out_weight,
    norm_gain,
    gate_weight,
    up_weight,
    down_weight,
    routes,
    route_weight,
):
    weight_of = gathered_by_doubling(out_weight, "tp")
    tok_count = query_rows.shape[0]
    head_local = query_rows.shape[1] // HDIM
    group_local = key_rows.shape[1] // HDIM
    repeat = head_local // group_local
    first_pos = lax.axis_index("sp") * tok_count
    positions = first_pos + jnp.arange(tok_count, dtype=jnp.int32)
    rot_q = rotate(query_rows, positions, head_local)
    rot_k = rotate(key_rows, positions, group_local)
    tails = jnp.stack([rot_k[tok_count - WINDOW :], value_rows[tok_count - WINDOW :]])
    earlier = shifted(tails, "sp", 1)
    blocks = tok_count // WINDOW
    q_blocks = rot_q.reshape(blocks, WINDOW, group_local, repeat, HDIM)
    k_blocks = rot_k.reshape(blocks, WINDOW, group_local, HDIM)
    v_blocks = value_rows.reshape(blocks, WINDOW, group_local, HDIM)
    k_prev = jnp.concatenate(
        [earlier[0].reshape(1, WINDOW, group_local, HDIM), k_blocks[:-1]], axis=0
    )
    v_prev = jnp.concatenate(
        [earlier[1].reshape(1, WINDOW, group_local, HDIM), v_blocks[:-1]], axis=0
    )
    k_wide = jnp.concatenate([k_prev, k_blocks], axis=1)
    v_wide = jnp.concatenate([v_prev, v_blocks], axis=1)
    query_pos = jnp.arange(WINDOW) + WINDOW
    key_pos = jnp.arange(2 * WINDOW)
    distance = query_pos[:, None] - key_pos[None, :]
    in_band = (distance >= 0) & (distance < WINDOW)
    key_global = (
        first_pos + jnp.arange(blocks)[:, None, None] * WINDOW + key_pos[None, None, :] - WINDOW
    )
    allowed = in_band[None] & (key_global >= 0)
    scores = jnp.einsum(
        "nqgrd,nkgd->grnqk", q_blocks, k_wide, preferred_element_type=jnp.float32
    ) * HDIM ** (-0.5)
    scores = jnp.where(allowed[None, None], scores, -jnp.inf)
    sink_here = sink_logits.reshape(group_local, repeat)[:, :, None, None, None]
    largest = jnp.maximum(scores.max(axis=-1, keepdims=True), sink_here)
    exp_scores = jnp.exp(scores - largest)
    denominator = exp_scores.sum(axis=-1, keepdims=True) + jnp.exp(sink_here - largest)
    probs = (exp_scores / denominator).astype(jnp.bfloat16)
    attended = jnp.einsum("grnqk,nkgd->nqgrd", probs, v_wide, preferred_element_type=jnp.float32)
    attended = attended.astype(jnp.bfloat16).reshape(tok_count, head_local * HDIM)
    row_count = residual.shape[0]
    heads_wide = attended.shape[1]
    token_rows = lax.all_to_all(attended, "tp", split_axis=0, concat_axis=1, tiled=True)
    here = lax.axis_index("tp")
    projected = 0.0
    for offset in sorted(weight_of):
        part = lax.dynamic_slice_in_dim(token_rows, (here ^ offset) * heads_wide, heads_wide, 1)
        projected = projected + jnp.dot(
            part, weight_of[offset], preferred_element_type=jnp.float32
        )
    stream_f = (residual.astype(jnp.float32) + projected).astype(jnp.bfloat16).astype(jnp.float32)
    normed = (
        stream_f
        * lax.rsqrt(jnp.mean(stream_f * stream_f, axis=-1, keepdims=True) + norm_eps)
        * norm_gain[None, :]
    ).astype(jnp.bfloat16)
    sp_count = lax.axis_size("sp")
    tp_count = lax.axis_size("tp")
    expert_count = sp_count * tp_count
    capacity = 4 * row_count // expert_count
    width = normed.shape[1]
    slot_index = slots_of(routes, expert_count, capacity)
    slot_ids = jnp.arange(expert_count * capacity, dtype=jnp.int32)
    place = (slot_index[:, :, None] == slot_ids[None, None, :]).astype(jnp.bfloat16)
    outgoing = jnp.einsum(
        "ns,nd->sd", place[:, 0] + place[:, 1], normed, preferred_element_type=jnp.float32
    ).astype(jnp.bfloat16)
    outgoing = outgoing.reshape(expert_count, capacity, width)
    arrived = lax.all_to_all(outgoing, ("sp", "tp"), split_axis=0, concat_axis=0, tiled=True)
    flat_rows = arrived.reshape(-1, width)
    gate_out = jnp.dot(flat_rows, gate_weight[0], preferred_element_type=jnp.float32)
    up_out = jnp.dot(flat_rows, up_weight[0], preferred_element_type=jnp.float32)
    hidden = (jax.nn.silu(gate_out) * up_out).astype(jnp.bfloat16)
    produced = jnp.dot(hidden, down_weight[0], preferred_element_type=jnp.float32).astype(
        jnp.bfloat16
    )
    returned = lax.all_to_all(
        produced.reshape(arrived.shape), ("sp", "tp"), split_axis=0, concat_axis=0, tiled=True
    )
    returned = returned.reshape(expert_count * capacity, width)
    total = stream_f
    for k in range(2):
        picked = jnp.dot(place[:, k], returned, preferred_element_type=jnp.float32)
        total = total + picked * route_weight[:, k : k + 1]
    return total.astype(jnp.bfloat16)


def solution(mesh):
    in_specs = (
        P(("grp", "sp"), "tp"),
        P(("grp", "sp"), "tp"),
        P(("grp", "sp"), "tp"),
        P("tp"),
        P(("grp", "sp", "tp"), None),
        P("tp", None),
        P(),
        P(("sp", "tp"), None, None),
        P(("sp", "tp"), None, None),
        P(("sp", "tp"), None, None),
        P(("grp", "sp", "tp"), None),
        P(("grp", "sp", "tp"), None),
    )
    out_specs = P(("grp", "sp", "tp"), None)
    return jax.shard_map(
        per_device, mesh=mesh, in_specs=in_specs, out_specs=out_specs, check_vma=False
    )
```

```python
import jax
import jax.numpy as jnp
from jax import lax
from jax.sharding import PartitionSpec as P

HDIM = 64
WINDOW = 128
GROUPS = 4


rope_base = 10000.0
norm_eps = 1e-06


def shifted(block, axis, distance):
    devices = range(lax.axis_size(axis))
    route = [(i - distance, i) for i in devices if i - distance in devices]
    return lax.ppermute(block, axis, route)


def swapped(block, axis, offset):
    return lax.ppermute(block, axis, [(i, i ^ offset) for i in range(lax.axis_size(axis))])


def gathered_by_doubling(block, axis):
    blocks = {0: block}
    offset = lax.axis_size(axis) // 2
    while offset:
        blocks.update({m ^ offset: swapped(b, axis, offset) for m, b in blocks.items()})
        offset //= 2
    return blocks


def slots_of(routes, expert_count, capacity):
    count = routes.shape[0]
    experts = jnp.arange(expert_count, dtype=jnp.int32)
    named = (routes[:, :, None] == experts[None, None, :]).astype(jnp.bfloat16)
    either = named[:, 0] + named[:, 1]
    row = jnp.arange(count, dtype=jnp.int32)
    earlier = (row[:, None] > row[None, :]).astype(jnp.bfloat16)
    before = jnp.dot(earlier, either, preferred_element_type=jnp.float32)
    rank = jnp.sum(before[:, None, :] * named.astype(jnp.float32), axis=-1).astype(jnp.int32)
    return routes * capacity + rank


def turned_by(block, axis, distance):
    count = lax.axis_size(axis)
    return lax.ppermute(block, axis, [(i, (i + distance) % count) for i in range(count)])


def rotate(rows, positions, heads):
    half_dim = HDIM // 2
    values = rows.astype(jnp.float32).reshape(rows.shape[0], heads, HDIM)
    inverse = rope_base ** (-jnp.arange(half_dim, dtype=jnp.float32) / half_dim)
    angles = positions.astype(jnp.float32)[:, None] * inverse[None, :]
    cosines = jnp.cos(angles)[:, None, :]
    sines = jnp.sin(angles)[:, None, :]
    lower = values[..., :half_dim]
    upper = values[..., half_dim:]
    turned = jnp.concatenate(
        [lower * cosines - upper * sines, upper * cosines + lower * sines], axis=-1
    )
    return turned.reshape(rows.shape[0], heads * HDIM).astype(jnp.bfloat16)


def plan_planes(routes, route_weight):
    planes, lanes = lax.axis_size("sp"), lax.axis_size("tp")
    plane, lane = lax.axis_index("sp"), lax.axis_index("tp")
    count = routes.shape[0]
    rows = lanes * (4 * count // (planes * lanes)) // 2
    capacity = 4 * count // (planes * lanes)
    meta = jnp.concatenate([routes.astype(jnp.float32), route_weight], axis=1).T
    metas = jnp.stack([meta] + [turned_by(meta, "sp", d) for d in range(1, planes)])
    row = jnp.arange(count, dtype=jnp.int32)
    earlier = (row[:, None] < row[None, :]).astype(jnp.bfloat16)

    def ranked(named):
        return jnp.einsum(
            "...tm,mn->...tn", named.astype(jnp.bfloat16), earlier, preferred_element_type=jnp.float32
        )

    own = routes[:, 0] // lanes
    in_plane = jnp.arange(planes, dtype=jnp.int32)[:, None] == own[None, :]
    own_rank = jnp.sum(jnp.where(in_plane, ranked(in_plane), 0.0), axis=0).astype(jnp.int32)
    key = lax.rem(own - plane + planes, planes) * rows + own_rank
    send = (jnp.arange(planes * rows, dtype=jnp.int32)[:, None] == key[None, :]).astype(jnp.bfloat16)

    experts = metas[:, :2].astype(jnp.int32)
    mine = experts[:, 0] // lanes == plane
    local = lax.rem(experts, lanes)
    named = (local[:, :, None, :] == jnp.arange(lanes, dtype=jnp.int32)[:, None]) & mine[:, None, None]
    before = ranked(named[:, 0] | named[:, 1])
    rank = jnp.sum(jnp.where(named, before[:, None], 0.0), axis=2).astype(jnp.int32)
    slot = jnp.where(mine[:, None], (local ^ lane) * capacity + rank, -1)
    spot = slot[:, :, None, :] == jnp.arange(lanes * capacity, dtype=jnp.int32)[:, None]
    mine_rank = ranked(mine[:, None])[:, 0].astype(jnp.int32)
    line = (mine_rank[:, None] == jnp.arange(rows, dtype=jnp.int32)[:, None]) & mine[:, None]
    spread = jnp.einsum(
        "dsn,drn->dsr",
        (spot[:, 0] | spot[:, 1]).astype(jnp.bfloat16),
        line.astype(jnp.bfloat16),
        preferred_element_type=jnp.float32,
    ).astype(jnp.bfloat16)
    weighted = jnp.sum(jnp.where(spot, metas[:, 2:, None], 0.0), axis=1)
    fold = jnp.einsum(
        "drn,dsn->drs",
        line.astype(jnp.float32),
        weighted,
        precision=lax.Precision.HIGHEST,
        preferred_element_type=jnp.float32,
    )
    coarse = fold.astype(jnp.bfloat16)
    fine = (fold - coarse.astype(jnp.float32)).astype(jnp.bfloat16)
    return send, spread, coarse, fine


def lane_exchange(blocks):
    offset = lax.axis_size("tp") // 2
    while offset:
        keep = [m for m in sorted(blocks) if not m & offset]
        go = [m for m in sorted(blocks) if m & offset]
        size = blocks[0].shape[0]
        came = swapped(jnp.concatenate([blocks[m] for m in go]), "tp", offset)
        for i, m in enumerate(go):
            blocks[m] = came[i * size : (i + 1) * size]
        offset //= 2
    return blocks


def plane_experts(stream_f, normed, plans, gate, up, down):
    send, spread, coarse, fine = plans
    planes, lanes = lax.axis_size("sp"), lax.axis_size("tp")
    rows = send.shape[0] // planes
    capacity = spread.shape[1] // lanes
    leaving = jnp.dot(send, normed, preferred_element_type=jnp.float32).astype(jnp.bfloat16)
    came = [leaving[:rows]]
    for d in range(1, planes):
        came.append(turned_by(leaving[d * rows : (d + 1) * rows], "sp", d))

    def lanes_apart(block):
        return {m: block[m * capacity : (m + 1) * capacity] for m in range(lanes)}

    def joined(blocks):
        return jnp.concatenate([blocks[m] for m in range(lanes)])

    back = []
    for d in range(planes):
        slots = jnp.dot(spread[d], came[d], preferred_element_type=jnp.float32)
        served = joined(lane_exchange(lanes_apart(slots.astype(jnp.bfloat16))))
        gate_out = jnp.dot(served, gate, preferred_element_type=jnp.float32)
        up_out = jnp.dot(served, up, preferred_element_type=jnp.float32)
        hidden = (jax.nn.silu(gate_out) * up_out).astype(jnp.bfloat16)
        produced = jnp.dot(hidden, down, preferred_element_type=jnp.float32).astype(jnp.bfloat16)
        returned = joined(lane_exchange(lanes_apart(produced)))
        folded = jnp.dot(coarse[d], returned, preferred_element_type=jnp.float32)
        folded = folded + jnp.dot(fine[d], returned, preferred_element_type=jnp.float32)
        folded = folded.astype(jnp.bfloat16)
        back.append(turned_by(folded, "sp", planes - d) if d else folded)
    total = stream_f
    for d in range(planes):
        total = total + jnp.einsum(
            "rn,rd->nd",
            send[d * rows : (d + 1) * rows],
            back[d],
            preferred_element_type=jnp.float32,
        )
    return total.astype(jnp.bfloat16)


def direct_experts(stream_f, normed, plans, gate, up, down, routes, route_weight):
    row_count = normed.shape[0]
    sp_count = lax.axis_size("sp")
    tp_count = lax.axis_size("tp")
    expert_count = sp_count * tp_count
    capacity = 4 * row_count // expert_count
    width = normed.shape[1]
    slot_index = slots_of(routes, expert_count, capacity)
    slot_ids = jnp.arange(expert_count * capacity, dtype=jnp.int32)
    place = (slot_index[:, :, None] == slot_ids[None, None, :]).astype(jnp.bfloat16)
    outgoing = jnp.einsum(
        "ns,nd->sd", place[:, 0] + place[:, 1], normed, preferred_element_type=jnp.float32
    ).astype(jnp.bfloat16)
    outgoing = outgoing.reshape(expert_count, capacity, width)
    arrived = lax.all_to_all(outgoing, ("sp", "tp"), split_axis=0, concat_axis=0, tiled=True)
    flat_rows = arrived.reshape(-1, width)
    gate_out = jnp.dot(flat_rows, gate, preferred_element_type=jnp.float32)
    up_out = jnp.dot(flat_rows, up, preferred_element_type=jnp.float32)
    hidden = (jax.nn.silu(gate_out) * up_out).astype(jnp.bfloat16)
    produced = jnp.dot(hidden, down, preferred_element_type=jnp.float32).astype(
        jnp.bfloat16
    )
    returned = lax.all_to_all(
        produced.reshape(arrived.shape), ("sp", "tp"), split_axis=0, concat_axis=0, tiled=True
    )
    returned = returned.reshape(expert_count * capacity, width)
    total = stream_f
    for k in range(2):
        picked = jnp.dot(place[:, k], returned, preferred_element_type=jnp.float32)
        total = total + picked * route_weight[:, k : k + 1]
    return total.astype(jnp.bfloat16)


def per_device(
    query_rows,
    key_rows,
    value_rows,
    sink_logits,
    residual,
    out_weight,
    norm_gain,
    gate_weight,
    up_weight,
    down_weight,
    routes,
    route_weight,
):
    plans = plan_planes(routes, route_weight) if lax.axis_size("sp") == GROUPS else None
    weight_of = gathered_by_doubling(out_weight, "tp")
    tok_count = query_rows.shape[0]
    head_local = query_rows.shape[1] // HDIM
    group_local = key_rows.shape[1] // HDIM
    repeat = head_local // group_local
    first_pos = lax.axis_index("sp") * tok_count
    positions = first_pos + jnp.arange(tok_count, dtype=jnp.int32)
    rot_q = rotate(query_rows, positions, head_local)
    rot_k = rotate(key_rows, positions, group_local)
    tails = jnp.stack([rot_k[tok_count - WINDOW :], value_rows[tok_count - WINDOW :]])
    earlier = shifted(tails, "sp", 1)
    blocks = tok_count // WINDOW
    q_blocks = rot_q.reshape(blocks, WINDOW, group_local, repeat, HDIM)
    k_blocks = rot_k.reshape(blocks, WINDOW, group_local, HDIM)
    v_blocks = value_rows.reshape(blocks, WINDOW, group_local, HDIM)
    k_prev = jnp.concatenate(
        [earlier[0].reshape(1, WINDOW, group_local, HDIM), k_blocks[:-1]], axis=0
    )
    v_prev = jnp.concatenate(
        [earlier[1].reshape(1, WINDOW, group_local, HDIM), v_blocks[:-1]], axis=0
    )
    k_wide = jnp.concatenate([k_prev, k_blocks], axis=1)
    v_wide = jnp.concatenate([v_prev, v_blocks], axis=1)
    query_pos = jnp.arange(WINDOW) + WINDOW
    key_pos = jnp.arange(2 * WINDOW)
    distance = query_pos[:, None] - key_pos[None, :]
    in_band = (distance >= 0) & (distance < WINDOW)
    key_global = (
        first_pos + jnp.arange(blocks)[:, None, None] * WINDOW + key_pos[None, None, :] - WINDOW
    )
    allowed = in_band[None] & (key_global >= 0)
    scores = jnp.einsum(
        "nqgrd,nkgd->grnqk", q_blocks, k_wide, preferred_element_type=jnp.float32
    ) * HDIM ** (-0.5)
    scores = jnp.where(allowed[None, None], scores, -jnp.inf)
    sink_here = sink_logits.reshape(group_local, repeat)[:, :, None, None, None]
    largest = jnp.maximum(scores.max(axis=-1, keepdims=True), sink_here)
    exp_scores = jnp.exp(scores - largest)
    denominator = exp_scores.sum(axis=-1, keepdims=True) + jnp.exp(sink_here - largest)
    probs = (exp_scores / denominator).astype(jnp.bfloat16)
    attended = jnp.einsum("grnqk,nkgd->nqgrd", probs, v_wide, preferred_element_type=jnp.float32)
    attended = attended.astype(jnp.bfloat16).reshape(tok_count, head_local * HDIM)
    row_count = residual.shape[0]
    heads_wide = attended.shape[1]
    token_rows = lax.all_to_all(attended, "tp", split_axis=0, concat_axis=1, tiled=True)
    here = lax.axis_index("tp")
    projected = 0.0
    for offset in sorted(weight_of):
        part = lax.dynamic_slice_in_dim(token_rows, (here ^ offset) * heads_wide, heads_wide, 1)
        projected = projected + jnp.dot(
            part, weight_of[offset], preferred_element_type=jnp.float32
        )
    stream_f = (residual.astype(jnp.float32) + projected).astype(jnp.bfloat16).astype(jnp.float32)
    normed = (
        stream_f
        * lax.rsqrt(jnp.mean(stream_f * stream_f, axis=-1, keepdims=True) + norm_eps)
        * norm_gain[None, :]
    ).astype(jnp.bfloat16)
    args = (stream_f, normed, plans, gate_weight[0], up_weight[0], down_weight[0])
    if lax.axis_size("sp") == GROUPS:
        return plane_experts(*args)
    return direct_experts(*args, routes, route_weight)


def solution(mesh):
    in_specs = (
        P(("grp", "sp"), "tp"),
        P(("grp", "sp"), "tp"),
        P(("grp", "sp"), "tp"),
        P("tp"),
        P(("grp", "sp", "tp"), None),
        P("tp", None),
        P(),
        P(("sp", "tp"), None, None),
        P(("sp", "tp"), None, None),
        P(("sp", "tp"), None, None),
        P(("grp", "sp", "tp"), None),
        P(("grp", "sp", "tp"), None),
    )
    out_specs = P(("grp", "sp", "tp"), None)
    return jax.shard_map(
        per_device, mesh=mesh, in_specs=in_specs, out_specs=out_specs, check_vma=False
    )
```

```python
import jax
import jax.numpy as jnp
from jax import lax
from jax.experimental import pallas as pl
from jax.experimental.pallas import tpu as pltpu
from jax.sharding import PartitionSpec as P

HDIM = 64
WINDOW = 128
GROUPS = 4


rope_base = 10000.0
norm_eps = 1e-06


def shifted(block, axis, distance):
    devices = range(lax.axis_size(axis))
    route = [(i - distance, i) for i in devices if i - distance in devices]
    return lax.ppermute(block, axis, route)


def swapped(block, axis, offset):
    return lax.ppermute(block, axis, [(i, i ^ offset) for i in range(lax.axis_size(axis))])


def gathered_by_doubling(block, axis):
    blocks = {0: block}
    offset = lax.axis_size(axis) // 2
    while offset:
        blocks.update({m ^ offset: swapped(b, axis, offset) for m, b in blocks.items()})
        offset //= 2
    return blocks


def slots_of(routes, expert_count, capacity):
    count = routes.shape[0]
    experts = jnp.arange(expert_count, dtype=jnp.int32)
    named = (routes[:, :, None] == experts[None, None, :]).astype(jnp.bfloat16)
    either = named[:, 0] + named[:, 1]
    row = jnp.arange(count, dtype=jnp.int32)
    earlier = (row[:, None] > row[None, :]).astype(jnp.bfloat16)
    before = jnp.dot(earlier, either, preferred_element_type=jnp.float32)
    rank = jnp.sum(before[:, None, :] * named.astype(jnp.float32), axis=-1).astype(jnp.int32)
    return routes * capacity + rank


def turned_by(block, axis, distance):
    count = lax.axis_size(axis)
    return lax.ppermute(block, axis, [(i, (i + distance) % count) for i in range(count)])


def rotate(rows, positions, heads):
    half_dim = HDIM // 2
    values = rows.astype(jnp.float32).reshape(rows.shape[0], heads, HDIM)
    inverse = rope_base ** (-jnp.arange(half_dim, dtype=jnp.float32) / half_dim)
    angles = positions.astype(jnp.float32)[:, None] * inverse[None, :]
    cosines = jnp.cos(angles)[:, None, :]
    sines = jnp.sin(angles)[:, None, :]
    lower = values[..., :half_dim]
    upper = values[..., half_dim:]
    turned = jnp.concatenate(
        [lower * cosines - upper * sines, upper * cosines + lower * sines], axis=-1
    )
    return turned.reshape(rows.shape[0], heads * HDIM).astype(jnp.bfloat16)


def plan_planes(routes, route_weight):
    planes, lanes = lax.axis_size("sp"), lax.axis_size("tp")
    plane, lane = lax.axis_index("sp"), lax.axis_index("tp")
    count = routes.shape[0]
    rows = lanes * (4 * count // (planes * lanes)) // 2
    capacity = 4 * count // (planes * lanes)
    meta = jnp.concatenate([routes.astype(jnp.float32), route_weight], axis=1).T
    metas = jnp.stack([meta] + [turned_by(meta, "sp", d) for d in range(1, planes)])
    row = jnp.arange(count, dtype=jnp.int32)
    earlier = (row[:, None] < row[None, :]).astype(jnp.bfloat16)

    def ranked(named):
        return jnp.einsum(
            "...tm,mn->...tn", named.astype(jnp.bfloat16), earlier, preferred_element_type=jnp.float32
        )

    own = routes[:, 0] // lanes
    in_plane = jnp.arange(planes, dtype=jnp.int32)[:, None] == own[None, :]
    own_rank = jnp.sum(jnp.where(in_plane, ranked(in_plane), 0.0), axis=0).astype(jnp.int32)
    key = lax.rem(own - plane + planes, planes) * rows + own_rank
    send = (jnp.arange(planes * rows, dtype=jnp.int32)[:, None] == key[None, :]).astype(jnp.bfloat16)

    experts = metas[:, :2].astype(jnp.int32)
    mine = experts[:, 0] // lanes == plane
    local = lax.rem(experts, lanes)
    named = (local[:, :, None, :] == jnp.arange(lanes, dtype=jnp.int32)[:, None]) & mine[:, None, None]
    before = ranked(named[:, 0] | named[:, 1])
    rank = jnp.sum(jnp.where(named, before[:, None], 0.0), axis=2).astype(jnp.int32)
    slot = jnp.where(mine[:, None], (local ^ lane) * capacity + rank, -1)
    spot = slot[:, :, None, :] == jnp.arange(lanes * capacity, dtype=jnp.int32)[:, None]
    mine_rank = ranked(mine[:, None])[:, 0].astype(jnp.int32)
    line = (mine_rank[:, None] == jnp.arange(rows, dtype=jnp.int32)[:, None]) & mine[:, None]
    spread = jnp.einsum(
        "dsn,drn->dsr",
        (spot[:, 0] | spot[:, 1]).astype(jnp.bfloat16),
        line.astype(jnp.bfloat16),
        preferred_element_type=jnp.float32,
    ).astype(jnp.bfloat16)
    weighted = jnp.sum(jnp.where(spot, metas[:, 2:, None], 0.0), axis=1)
    fold = jnp.einsum(
        "drn,dsn->drs",
        line.astype(jnp.float32),
        weighted,
        precision=lax.Precision.HIGHEST,
        preferred_element_type=jnp.float32,
    )
    coarse = fold.astype(jnp.bfloat16)
    fine = (fold - coarse.astype(jnp.float32)).astype(jnp.bfloat16)
    return send, spread, coarse, fine


def local_call(body, outs, flops, *operands):
    moved = sum(o.size * o.dtype.itemsize for o in list(operands) + list(outs))
    return pl.pallas_call(
        body,
        out_shape=tuple(outs),
        in_specs=[pl.BlockSpec(memory_space=pltpu.VMEM)] * len(operands),
        out_specs=tuple(pl.BlockSpec(memory_space=pltpu.VMEM) for _ in outs),
        cost_estimate=pl.CostEstimate(flops=flops, bytes_accessed=moved, transcendentals=0),
    )(*operands)


def split_lanes(spread, block, lanes):
    def body(spread_ref, block_ref, *out_refs):
        slots = jnp.dot(spread_ref[...], block_ref[...], preferred_element_type=jnp.float32)
        size = slots.shape[0] // lanes
        for m, out in enumerate(out_refs):
            out[...] = slots[m * size : (m + 1) * size].astype(out.dtype)

    piece = jax.ShapeDtypeStruct((spread.shape[0] // lanes, block.shape[1]), block.dtype)
    return local_call(body, [piece] * lanes, 2 * spread.size * block.shape[1], spread, block)


def serve(pieces, gate, up, down):
    count, size = len(pieces), pieces[0].shape[0]

    def body(*refs):
        ins, (gate_ref, up_ref, down_ref), outs = refs[:count], refs[count : count + 3], refs[count + 3 :]
        rows = jnp.concatenate([r[...] for r in ins], axis=0)
        gate_out = jnp.dot(rows, gate_ref[...], preferred_element_type=jnp.float32)
        up_out = jnp.dot(rows, up_ref[...], preferred_element_type=jnp.float32)
        hidden = (jax.nn.silu(gate_out) * up_out).astype(jnp.bfloat16)
        produced = jnp.dot(hidden, down_ref[...], preferred_element_type=jnp.float32)
        for m, out in enumerate(outs):
            out[...] = produced[m * size : (m + 1) * size].astype(out.dtype)

    outs = [jax.ShapeDtypeStruct(p.shape, p.dtype) for p in pieces]
    return local_call(body, outs, 6 * count * size * gate.size, *pieces, gate, up, down)


def fold_lanes(coarse, fine, pieces):
    def body(coarse_ref, fine_ref, *refs):
        rows = jnp.concatenate([r[...] for r in refs[:-1]], axis=0)
        total = jnp.dot(coarse_ref[...], rows, preferred_element_type=jnp.float32)
        total = total + jnp.dot(fine_ref[...], rows, preferred_element_type=jnp.float32)
        refs[-1][...] = total.astype(jnp.bfloat16)

    width = pieces[0].shape[1]
    out = jax.ShapeDtypeStruct((coarse.shape[0], width), jnp.bfloat16)
    return local_call(body, [out], 4 * coarse.size * width, coarse, fine, *pieces)[0]


def lane_exchange(pieces):
    return [swapped(p, "tp", m) if m else p for m, p in enumerate(pieces)]


def plane_experts(stream_f, normed, plans, gate, up, down):
    send, spread, coarse, fine = plans
    planes, lanes = lax.axis_size("sp"), lax.axis_size("tp")
    rows = send.shape[0] // planes
    came = []
    for d in range(planes):
        chunk = jnp.dot(
            send[d * rows : (d + 1) * rows], normed, preferred_element_type=jnp.float32
        ).astype(jnp.bfloat16)
        came.append(turned_by(chunk, "sp", d) if d else chunk)
    total = stream_f
    for batch in [(0, 1)] + [(d,) for d in range(2, planes)]:
        pieces = []
        for d in batch:
            pieces += lane_exchange(split_lanes(spread[d], came[d], lanes))
        produced = serve(pieces, gate, up, down)
        for i, d in enumerate(batch):
            returned = lane_exchange(produced[i * lanes : (i + 1) * lanes])
            folded = fold_lanes(coarse[d], fine[d], returned)
            back = turned_by(folded, "sp", planes - d) if d else folded
            total = total + jnp.einsum(
                "rn,rd->nd",
                send[d * rows : (d + 1) * rows],
                back,
                preferred_element_type=jnp.float32,
            )
    return total.astype(jnp.bfloat16)


def direct_experts(stream_f, normed, plans, gate, up, down, routes, route_weight):
    row_count = normed.shape[0]
    sp_count = lax.axis_size("sp")
    tp_count = lax.axis_size("tp")
    expert_count = sp_count * tp_count
    capacity = 4 * row_count // expert_count
    width = normed.shape[1]
    slot_index = slots_of(routes, expert_count, capacity)
    slot_ids = jnp.arange(expert_count * capacity, dtype=jnp.int32)
    place = (slot_index[:, :, None] == slot_ids[None, None, :]).astype(jnp.bfloat16)
    outgoing = jnp.einsum(
        "ns,nd->sd", place[:, 0] + place[:, 1], normed, preferred_element_type=jnp.float32
    ).astype(jnp.bfloat16)
    outgoing = outgoing.reshape(expert_count, capacity, width)
    arrived = lax.all_to_all(outgoing, ("sp", "tp"), split_axis=0, concat_axis=0, tiled=True)
    flat_rows = arrived.reshape(-1, width)
    gate_out = jnp.dot(flat_rows, gate, preferred_element_type=jnp.float32)
    up_out = jnp.dot(flat_rows, up, preferred_element_type=jnp.float32)
    hidden = (jax.nn.silu(gate_out) * up_out).astype(jnp.bfloat16)
    produced = jnp.dot(hidden, down, preferred_element_type=jnp.float32).astype(
        jnp.bfloat16
    )
    returned = lax.all_to_all(
        produced.reshape(arrived.shape), ("sp", "tp"), split_axis=0, concat_axis=0, tiled=True
    )
    returned = returned.reshape(expert_count * capacity, width)
    total = stream_f
    for k in range(2):
        picked = jnp.dot(place[:, k], returned, preferred_element_type=jnp.float32)
        total = total + picked * route_weight[:, k : k + 1]
    return total.astype(jnp.bfloat16)


def per_device(
    query_rows,
    key_rows,
    value_rows,
    sink_logits,
    residual,
    out_weight,
    norm_gain,
    gate_weight,
    up_weight,
    down_weight,
    routes,
    route_weight,
):
    plans = plan_planes(routes, route_weight) if lax.axis_size("sp") == GROUPS else None
    weight_of = gathered_by_doubling(out_weight, "tp")
    tok_count = query_rows.shape[0]
    head_local = query_rows.shape[1] // HDIM
    group_local = key_rows.shape[1] // HDIM
    repeat = head_local // group_local
    first_pos = lax.axis_index("sp") * tok_count
    positions = first_pos + jnp.arange(tok_count, dtype=jnp.int32)
    rot_q = rotate(query_rows, positions, head_local)
    rot_k = rotate(key_rows, positions, group_local)
    tails = jnp.stack([rot_k[tok_count - WINDOW :], value_rows[tok_count - WINDOW :]])
    earlier = shifted(tails, "sp", 1)
    blocks = tok_count // WINDOW
    q_blocks = rot_q.reshape(blocks, WINDOW, group_local, repeat, HDIM)
    k_blocks = rot_k.reshape(blocks, WINDOW, group_local, HDIM)
    v_blocks = value_rows.reshape(blocks, WINDOW, group_local, HDIM)
    k_prev = jnp.concatenate(
        [earlier[0].reshape(1, WINDOW, group_local, HDIM), k_blocks[:-1]], axis=0
    )
    v_prev = jnp.concatenate(
        [earlier[1].reshape(1, WINDOW, group_local, HDIM), v_blocks[:-1]], axis=0
    )
    k_wide = jnp.concatenate([k_prev, k_blocks], axis=1)
    v_wide = jnp.concatenate([v_prev, v_blocks], axis=1)
    query_pos = jnp.arange(WINDOW) + WINDOW
    key_pos = jnp.arange(2 * WINDOW)
    distance = query_pos[:, None] - key_pos[None, :]
    in_band = (distance >= 0) & (distance < WINDOW)
    key_global = (
        first_pos + jnp.arange(blocks)[:, None, None] * WINDOW + key_pos[None, None, :] - WINDOW
    )
    allowed = in_band[None] & (key_global >= 0)
    scores = jnp.einsum(
        "nqgrd,nkgd->grnqk", q_blocks, k_wide, preferred_element_type=jnp.float32
    ) * HDIM ** (-0.5)
    scores = jnp.where(allowed[None, None], scores, -jnp.inf)
    sink_here = sink_logits.reshape(group_local, repeat)[:, :, None, None, None]
    largest = jnp.maximum(scores.max(axis=-1, keepdims=True), sink_here)
    exp_scores = jnp.exp(scores - largest)
    denominator = exp_scores.sum(axis=-1, keepdims=True) + jnp.exp(sink_here - largest)
    probs = (exp_scores / denominator).astype(jnp.bfloat16)
    attended = jnp.einsum("grnqk,nkgd->nqgrd", probs, v_wide, preferred_element_type=jnp.float32)
    attended = attended.astype(jnp.bfloat16).reshape(tok_count, head_local * HDIM)
    row_count = residual.shape[0]
    heads_wide = attended.shape[1]
    token_rows = lax.all_to_all(attended, "tp", split_axis=0, concat_axis=1, tiled=True)
    here = lax.axis_index("tp")
    projected = 0.0
    for offset in sorted(weight_of):
        part = lax.dynamic_slice_in_dim(token_rows, (here ^ offset) * heads_wide, heads_wide, 1)
        projected = projected + jnp.dot(
            part, weight_of[offset], preferred_element_type=jnp.float32
        )
    stream_f = (residual.astype(jnp.float32) + projected).astype(jnp.bfloat16).astype(jnp.float32)
    normed = (
        stream_f
        * lax.rsqrt(jnp.mean(stream_f * stream_f, axis=-1, keepdims=True) + norm_eps)
        * norm_gain[None, :]
    ).astype(jnp.bfloat16)
    args = (stream_f, normed, plans, gate_weight[0], up_weight[0], down_weight[0])
    if lax.axis_size("sp") == GROUPS:
        return plane_experts(*args)
    return direct_experts(*args, routes, route_weight)


def solution(mesh):
    in_specs = (
        P(("grp", "sp"), "tp"),
        P(("grp", "sp"), "tp"),
        P(("grp", "sp"), "tp"),
        P("tp"),
        P(("grp", "sp", "tp"), None),
        P("tp", None),
        P(),
        P(("sp", "tp"), None, None),
        P(("sp", "tp"), None, None),
        P(("sp", "tp"), None, None),
        P(("grp", "sp", "tp"), None),
        P(("grp", "sp", "tp"), None),
    )
    out_specs = P(("grp", "sp", "tp"), None)
    return jax.shard_map(
        per_device, mesh=mesh, in_specs=in_specs, out_specs=out_specs, check_vma=False
    )
```

```python
import jax
import jax.numpy as jnp
from jax import lax
from jax.experimental import pallas as pl
from jax.experimental.pallas import tpu as pltpu
from jax.sharding import PartitionSpec as P

HDIM = 64
WINDOW = 128
GROUPS = 4


rope_base = 10000.0
norm_eps = 1e-06


def shifted(block, axis, distance):
    devices = range(lax.axis_size(axis))
    route = [(i - distance, i) for i in devices if i - distance in devices]
    return lax.ppermute(block, axis, route)


def swapped(block, axis, offset):
    return lax.ppermute(block, axis, [(i, i ^ offset) for i in range(lax.axis_size(axis))])


def gathered_by_doubling(block, axis):
    blocks = {0: block}
    offset = lax.axis_size(axis) // 2
    while offset:
        blocks.update({m ^ offset: swapped(b, axis, offset) for m, b in blocks.items()})
        offset //= 2
    return blocks


def slots_of(routes, expert_count, capacity):
    count = routes.shape[0]
    experts = jnp.arange(expert_count, dtype=jnp.int32)
    named = (routes[:, :, None] == experts[None, None, :]).astype(jnp.bfloat16)
    either = named[:, 0] + named[:, 1]
    row = jnp.arange(count, dtype=jnp.int32)
    earlier = (row[:, None] > row[None, :]).astype(jnp.bfloat16)
    before = jnp.dot(earlier, either, preferred_element_type=jnp.float32)
    rank = jnp.sum(before[:, None, :] * named.astype(jnp.float32), axis=-1).astype(jnp.int32)
    return routes * capacity + rank


def turned_by(block, axis, distance):
    count = lax.axis_size(axis)
    return lax.ppermute(block, axis, [(i, (i + distance) % count) for i in range(count)])


def rotate(rows, positions, heads):
    half_dim = HDIM // 2
    values = rows.astype(jnp.float32).reshape(rows.shape[0], heads, HDIM)
    inverse = rope_base ** (-jnp.arange(half_dim, dtype=jnp.float32) / half_dim)
    angles = positions.astype(jnp.float32)[:, None] * inverse[None, :]
    cosines = jnp.cos(angles)[:, None, :]
    sines = jnp.sin(angles)[:, None, :]
    lower = values[..., :half_dim]
    upper = values[..., half_dim:]
    turned = jnp.concatenate(
        [lower * cosines - upper * sines, upper * cosines + lower * sines], axis=-1
    )
    return turned.reshape(rows.shape[0], heads * HDIM).astype(jnp.bfloat16)


def plan_planes(routes, route_weight):
    planes, lanes = lax.axis_size("sp"), lax.axis_size("tp")
    plane, lane = lax.axis_index("sp"), lax.axis_index("tp")
    count = routes.shape[0]
    rows = lanes * (4 * count // (planes * lanes)) // 2
    capacity = 4 * count // (planes * lanes)
    meta = jnp.concatenate([routes.astype(jnp.float32), route_weight], axis=1).T
    metas = jnp.stack([meta] + [turned_by(meta, "sp", d) for d in range(1, planes)])
    row = jnp.arange(count, dtype=jnp.int32)
    earlier = (row[:, None] < row[None, :]).astype(jnp.bfloat16)

    def ranked(named):
        return jnp.einsum(
            "...tm,mn->...tn", named.astype(jnp.bfloat16), earlier, preferred_element_type=jnp.float32
        )

    own = routes[:, 0] // lanes
    in_plane = jnp.arange(planes, dtype=jnp.int32)[:, None] == own[None, :]
    own_rank = jnp.sum(jnp.where(in_plane, ranked(in_plane), 0.0), axis=0).astype(jnp.int32)
    key = lax.rem(own - plane + planes, planes) * rows + own_rank
    send = (jnp.arange(planes * rows, dtype=jnp.int32)[:, None] == key[None, :]).astype(jnp.bfloat16)

    experts = metas[:, :2].astype(jnp.int32)
    mine = experts[:, 0] // lanes == plane
    local = lax.rem(experts, lanes)
    named = (local[:, :, None, :] == jnp.arange(lanes, dtype=jnp.int32)[:, None]) & mine[:, None, None]
    before = ranked(named[:, 0] | named[:, 1])
    rank = jnp.sum(jnp.where(named, before[:, None], 0.0), axis=2).astype(jnp.int32)
    slot = jnp.where(mine[:, None], (local ^ lane) * capacity + rank, -1)
    spot = slot[:, :, None, :] == jnp.arange(lanes * capacity, dtype=jnp.int32)[:, None]
    mine_rank = ranked(mine[:, None])[:, 0].astype(jnp.int32)
    line = (mine_rank[:, None] == jnp.arange(rows, dtype=jnp.int32)[:, None]) & mine[:, None]
    spread = jnp.einsum(
        "dsn,drn->dsr",
        (spot[:, 0] | spot[:, 1]).astype(jnp.bfloat16),
        line.astype(jnp.bfloat16),
        preferred_element_type=jnp.float32,
    ).astype(jnp.bfloat16)
    weighted = jnp.sum(jnp.where(spot, metas[:, 2:, None], 0.0), axis=1)
    fold = jnp.einsum(
        "drn,dsn->drs",
        line.astype(jnp.float32),
        weighted,
        precision=lax.Precision.HIGHEST,
        preferred_element_type=jnp.float32,
    )
    coarse = fold.astype(jnp.bfloat16)
    fine = (fold - coarse.astype(jnp.float32)).astype(jnp.bfloat16)
    return send, spread, coarse, fine


def local_call(body, outs, flops, *operands):
    moved = sum(o.size * o.dtype.itemsize for o in list(operands) + list(outs))
    return pl.pallas_call(
        body,
        out_shape=tuple(outs),
        in_specs=[pl.BlockSpec(memory_space=pltpu.VMEM)] * len(operands),
        out_specs=tuple(pl.BlockSpec(memory_space=pltpu.VMEM) for _ in outs),
        cost_estimate=pl.CostEstimate(flops=flops, bytes_accessed=moved, transcendentals=0),
    )(*operands)


def split_lanes(spread, block, lanes):
    def body(spread_ref, block_ref, *out_refs):
        slots = jnp.dot(spread_ref[...], block_ref[...], preferred_element_type=jnp.float32)
        size = slots.shape[0] // lanes
        for m, out in enumerate(out_refs):
            out[...] = slots[m * size : (m + 1) * size].astype(out.dtype)

    piece = jax.ShapeDtypeStruct((spread.shape[0] // lanes, block.shape[1]), block.dtype)
    return local_call(body, [piece] * lanes, 2 * spread.size * block.shape[1], spread, block)


def serve(pieces, gate, up, down):
    count, size = len(pieces), pieces[0].shape[0]

    def body(*refs):
        ins, (gate_ref, up_ref, down_ref), outs = refs[:count], refs[count : count + 3], refs[count + 3 :]
        rows = jnp.concatenate([r[...] for r in ins], axis=0)
        gate_out = jnp.dot(rows, gate_ref[...], preferred_element_type=jnp.float32)
        up_out = jnp.dot(rows, up_ref[...], preferred_element_type=jnp.float32)
        hidden = (jax.nn.silu(gate_out) * up_out).astype(jnp.bfloat16)
        produced = jnp.dot(hidden, down_ref[...], preferred_element_type=jnp.float32)
        for m, out in enumerate(outs):
            out[...] = produced[m * size : (m + 1) * size].astype(out.dtype)

    outs = [jax.ShapeDtypeStruct(p.shape, p.dtype) for p in pieces]
    return local_call(body, outs, 6 * count * size * gate.size, *pieces, gate, up, down)


def fold_lanes(coarse, fine, pieces):
    def body(coarse_ref, fine_ref, *refs):
        rows = jnp.concatenate([r[...] for r in refs[:-1]], axis=0)
        total = jnp.dot(coarse_ref[...], rows, preferred_element_type=jnp.float32)
        total = total + jnp.dot(fine_ref[...], rows, preferred_element_type=jnp.float32)
        refs[-1][...] = total.astype(jnp.bfloat16)

    width = pieces[0].shape[1]
    out = jax.ShapeDtypeStruct((coarse.shape[0], width), jnp.bfloat16)
    return local_call(body, [out], 4 * coarse.size * width, coarse, fine, *pieces)[0]


def lane_exchange(pieces):
    return [swapped(p, "tp", m) if m else p for m, p in enumerate(pieces)]


def plane_experts(stream_f, normed, plans, gate, up, down):
    send, spread, coarse, fine = plans
    planes, lanes = lax.axis_size("sp"), lax.axis_size("tp")
    rows = send.shape[0] // planes
    came = []
    for d in range(planes):
        chunk = jnp.dot(
            send[d * rows : (d + 1) * rows], normed, preferred_element_type=jnp.float32
        ).astype(jnp.bfloat16)
        came.append(turned_by(chunk, "sp", d) if d else chunk)
    total = stream_f
    for batch in [range(planes)[d : d + 2] for d in range(0, planes, 2)]:
        pieces = []
        for d in batch:
            pieces += lane_exchange(split_lanes(spread[d], came[d], lanes))
        produced = serve(pieces, gate, up, down)
        for i, d in enumerate(batch):
            returned = lane_exchange(produced[i * lanes : (i + 1) * lanes])
            folded = fold_lanes(coarse[d], fine[d], returned)
            back = turned_by(folded, "sp", planes - d) if d else folded
            total = total + jnp.einsum(
                "rn,rd->nd",
                send[d * rows : (d + 1) * rows],
                back,
                preferred_element_type=jnp.float32,
            )
    return total.astype(jnp.bfloat16)


def direct_experts(stream_f, normed, plans, gate, up, down, routes, route_weight):
    row_count = normed.shape[0]
    sp_count = lax.axis_size("sp")
    tp_count = lax.axis_size("tp")
    expert_count = sp_count * tp_count
    capacity = 4 * row_count // expert_count
    width = normed.shape[1]
    slot_index = slots_of(routes, expert_count, capacity)
    slot_ids = jnp.arange(expert_count * capacity, dtype=jnp.int32)
    place = (slot_index[:, :, None] == slot_ids[None, None, :]).astype(jnp.bfloat16)
    outgoing = jnp.einsum(
        "ns,nd->sd", place[:, 0] + place[:, 1], normed, preferred_element_type=jnp.float32
    ).astype(jnp.bfloat16)
    outgoing = outgoing.reshape(expert_count, capacity, width)
    arrived = lax.all_to_all(outgoing, ("sp", "tp"), split_axis=0, concat_axis=0, tiled=True)
    flat_rows = arrived.reshape(-1, width)
    gate_out = jnp.dot(flat_rows, gate, preferred_element_type=jnp.float32)
    up_out = jnp.dot(flat_rows, up, preferred_element_type=jnp.float32)
    hidden = (jax.nn.silu(gate_out) * up_out).astype(jnp.bfloat16)
    produced = jnp.dot(hidden, down, preferred_element_type=jnp.float32).astype(
        jnp.bfloat16
    )
    returned = lax.all_to_all(
        produced.reshape(arrived.shape), ("sp", "tp"), split_axis=0, concat_axis=0, tiled=True
    )
    returned = returned.reshape(expert_count * capacity, width)
    total = stream_f
    for k in range(2):
        picked = jnp.dot(place[:, k], returned, preferred_element_type=jnp.float32)
        total = total + picked * route_weight[:, k : k + 1]
    return total.astype(jnp.bfloat16)


def per_device(
    query_rows,
    key_rows,
    value_rows,
    sink_logits,
    residual,
    out_weight,
    norm_gain,
    gate_weight,
    up_weight,
    down_weight,
    routes,
    route_weight,
):
    plans = plan_planes(routes, route_weight) if lax.axis_size("sp") == GROUPS else None
    weight_of = gathered_by_doubling(out_weight, "tp")
    tok_count = query_rows.shape[0]
    head_local = query_rows.shape[1] // HDIM
    group_local = key_rows.shape[1] // HDIM
    repeat = head_local // group_local
    first_pos = lax.axis_index("sp") * tok_count
    positions = first_pos + jnp.arange(tok_count, dtype=jnp.int32)
    rot_q = rotate(query_rows, positions, head_local)
    rot_k = rotate(key_rows, positions, group_local)
    tails = jnp.stack([rot_k[tok_count - WINDOW :], value_rows[tok_count - WINDOW :]])
    earlier = shifted(tails, "sp", 1)
    blocks = tok_count // WINDOW
    q_blocks = rot_q.reshape(blocks, WINDOW, group_local, repeat, HDIM)
    k_blocks = rot_k.reshape(blocks, WINDOW, group_local, HDIM)
    v_blocks = value_rows.reshape(blocks, WINDOW, group_local, HDIM)
    k_prev = jnp.concatenate(
        [earlier[0].reshape(1, WINDOW, group_local, HDIM), k_blocks[:-1]], axis=0
    )
    v_prev = jnp.concatenate(
        [earlier[1].reshape(1, WINDOW, group_local, HDIM), v_blocks[:-1]], axis=0
    )
    k_wide = jnp.concatenate([k_prev, k_blocks], axis=1)
    v_wide = jnp.concatenate([v_prev, v_blocks], axis=1)
    query_pos = jnp.arange(WINDOW) + WINDOW
    key_pos = jnp.arange(2 * WINDOW)
    distance = query_pos[:, None] - key_pos[None, :]
    in_band = (distance >= 0) & (distance < WINDOW)
    key_global = (
        first_pos + jnp.arange(blocks)[:, None, None] * WINDOW + key_pos[None, None, :] - WINDOW
    )
    allowed = in_band[None] & (key_global >= 0)
    scores = jnp.einsum(
        "nqgrd,nkgd->grnqk", q_blocks, k_wide, preferred_element_type=jnp.float32
    ) * HDIM ** (-0.5)
    scores = jnp.where(allowed[None, None], scores, -jnp.inf)
    sink_here = sink_logits.reshape(group_local, repeat)[:, :, None, None, None]
    largest = jnp.maximum(scores.max(axis=-1, keepdims=True), sink_here)
    exp_scores = jnp.exp(scores - largest)
    denominator = exp_scores.sum(axis=-1, keepdims=True) + jnp.exp(sink_here - largest)
    probs = (exp_scores / denominator).astype(jnp.bfloat16)
    attended = jnp.einsum("grnqk,nkgd->nqgrd", probs, v_wide, preferred_element_type=jnp.float32)
    attended = attended.astype(jnp.bfloat16).reshape(tok_count, head_local * HDIM)
    row_count = residual.shape[0]
    heads_wide = attended.shape[1]
    token_rows = lax.all_to_all(attended, "tp", split_axis=0, concat_axis=1, tiled=True)
    here = lax.axis_index("tp")
    projected = 0.0
    for offset in sorted(weight_of):
        part = lax.dynamic_slice_in_dim(token_rows, (here ^ offset) * heads_wide, heads_wide, 1)
        projected = projected + jnp.dot(
            part, weight_of[offset], preferred_element_type=jnp.float32
        )
    stream_f = (residual.astype(jnp.float32) + projected).astype(jnp.bfloat16).astype(jnp.float32)
    normed = (
        stream_f
        * lax.rsqrt(jnp.mean(stream_f * stream_f, axis=-1, keepdims=True) + norm_eps)
        * norm_gain[None, :]
    ).astype(jnp.bfloat16)
    args = (stream_f, normed, plans, gate_weight[0], up_weight[0], down_weight[0])
    if lax.axis_size("sp") == GROUPS:
        return plane_experts(*args)
    return direct_experts(*args, routes, route_weight)


def solution(mesh):
    in_specs = (
        P(("grp", "sp"), "tp"),
        P(("grp", "sp"), "tp"),
        P(("grp", "sp"), "tp"),
        P("tp"),
        P(("grp", "sp", "tp"), None),
        P("tp", None),
        P(),
        P(("sp", "tp"), None, None),
        P(("sp", "tp"), None, None),
        P(("sp", "tp"), None, None),
        P(("grp", "sp", "tp"), None),
        P(("grp", "sp", "tp"), None),
    )
    out_specs = P(("grp", "sp", "tp"), None)
    return jax.shard_map(
        per_device, mesh=mesh, in_specs=in_specs, out_specs=out_specs, check_vma=False
    )
```
